256 devices in a mesh: sp: 32 (over z, x), dp: 8 (over y, core).
Axes of the slice: x: 4, y: 4, z: 8, core: 2. Of those that a mesh axis runs over, the one named last changes fastest.
Arguments:
- inputs: bfloat16 [8, 8192, 2048], P('dp', 'sp'), may hold values from -6 to 6
- up_pre: bfloat16 [8, 8192, 1024], P('dp', 'sp'), may hold values from -6 to 6
- gate_pre: bfloat16 [8, 8192, 1024], P('dp', 'sp'), may hold values from -6 to 6
- cotangent: bfloat16 [8, 8192, 1024], P('dp', 'sp'), may hold values from -6 to 6
- norm_gain: float32 [1024], replicated, may hold values from 0.1 to 1.9
- up_weight: bfloat16 [2048, 1024], P('dp'), may hold values from -0.125 to 0.125
- gate_weight: bfloat16 [2048, 1024], P('dp'), may hold values from -0.125 to 0.125
- mix_weight: bfloat16 [8, 512, 512], replicated, may hold values from -0.375 to 0.375
Outputs:
- input_grad: bfloat16 [8, 8192, 2048], P('dp', 'sp')
- up_weight_grad: float32 [2048, 1024], P('dp')
- gate_weight_grad: float32 [2048, 1024], P('dp')
The draws below stay inside these ranges and needn't reach their ends.
All inputs are finite; a program needn't handle non-finite values.
Results may differ from the reference program's by a relative error of at most 0.0064.
Values may be sent and summed in bfloat16 or wider, within the bound.
A program may use at most 128 MiB of HBM per device.

```python
import math
import jax
import jax.numpy as jnp
from jax import lax

MODEL = 2048
GROUPS = 8
GROUP_CH = 128
SPAN = 512
SEG = 64
GATED = 1024
LENGTH = 8192
BATCH = 8


def levels(stream_key, dims, pieces, smallest, high):
    loudness = 1.0
    for axis_at, parts in pieces:
        draws = jax.random.uniform(jax.random.fold_in(jax.random.fold_in(stream_key, 6), axis_at), (parts,), jnp.float32, smallest / len(pieces), high / len(pieces))
        loudness = loudness * jnp.repeat(jnp.exp(draws), dims[axis_at] // parts).reshape((-1,) + (1,) * (len(dims) - 1 - axis_at))
    return loudness


def noise(own_key, shape, deviation, reach, split=(), dtype=jnp.bfloat16):
    entries = deviation * jax.random.normal(own_key, shape, jnp.float32)
    if split:
        entries = entries * levels(own_key, shape, split, -0.22, 0.18)
    return jnp.clip(entries, -reach, reach).astype(dtype)


def setup_inputs(seed: int = 0) -> dict:
    key_list = jax.random.split(jax.random.key(seed), 9)
    inputs = noise(key_list[0], (BATCH, LENGTH, MODEL), 1.0, 6.0, ((0, 8), (1, 32)))
    up_pre = noise(key_list[1], (BATCH, LENGTH, GATED), 1.0, 6.0, ((0, 8), (1, 32)))
    gate_pre = noise(key_list[2], (BATCH, LENGTH, GATED), 1.0, 6.0, ((0, 8), (1, 32)))
    cotangent = noise(key_list[3], (BATCH, LENGTH, GATED), 1.0, 6.0, ((0, 8), (1, 32)))
    norm_gain = jnp.clip(1.0 + 0.18 * jax.random.normal(key_list[4], (GATED,), jnp.float32), 0.1, 1.9)
    up_weight = noise(key_list[5], (MODEL, GATED), MODEL ** -0.5, 0.125, ((0, 8),))
    gate_weight = noise(key_list[6], (MODEL, GATED), MODEL ** -0.5, 0.125, ((0, 8),))
    mix_weight = noise(key_list[7], (GROUPS, SPAN, SPAN), (SPAN // 2) ** -0.5, 0.375)
    return dict(inputs=inputs, up_pre=up_pre, gate_pre=gate_pre, cotangent=cotangent, norm_gain=norm_gain, up_weight=up_weight, gate_weight=gate_weight, mix_weight=mix_weight)


norm_eps = 1e-05
grad_scale = 1.0 / 256.0
root_half = 1.0 / math.sqrt(2.0)
root_twopi = 1.0 / math.sqrt(2.0 * math.pi)

def gelu_value(preact):
    return 0.5 * preact * (1.0 + lax.erf(preact * root_half))

def gelu_slope(preact):
    return 0.5 * (1.0 + lax.erf(preact * root_half)) + preact * jnp.exp(-0.5 * preact * preact) * root_twopi

def span_mask():
    segment = jnp.arange(SPAN) // SEG
    return segment[None, :] <= segment[:, None]

def reference(inputs, up_pre, gate_pre, cotangent, norm_gain, up_weight, gate_weight, mix_weight):
    up_float = up_pre.astype(jnp.float32)
    gate_float = gate_pre.astype(jnp.float32)
    grad_float = cotangent.astype(jnp.float32)
    gated_act = gelu_value(gate_float)
    centered = gated_act - lax.optimization_barrier(jnp.mean(gated_act, axis=-1, keepdims=True))
    inverse_std = lax.rsqrt(lax.optimization_barrier(jnp.mean(centered * centered, axis=-1, keepdims=True)) + norm_eps)
    normed = centered * inverse_std
    mixer_in = (normed * norm_gain).astype(jnp.bfloat16)
    mixer_grad = (grad_float * gelu_value(up_float)).astype(jnp.bfloat16)
    masked = jnp.where(span_mask()[None], mix_weight, jnp.zeros_like(mix_weight)).astype(jnp.float32)
    block_count = LENGTH // SPAN
    block_shape = (BATCH, block_count, SPAN, GROUPS, GROUP_CH)
    input_blocks = mixer_in.astype(jnp.float32).reshape(block_shape)
    grad_blocks = mixer_grad.astype(jnp.float32).reshape(block_shape)
    spatial = jnp.einsum('gts,bnsgc->bntgc', masked, input_blocks).astype(jnp.bfloat16)
    spatial = spatial.reshape(BATCH, LENGTH, GATED)
    normed_back = jnp.einsum('gts,bntgc->bnsgc', masked, grad_blocks).astype(jnp.bfloat16)
    normed_back = normed_back.reshape(BATCH, LENGTH, GATED)
    up_pre_grad = (grad_float * spatial.astype(jnp.float32) * gelu_slope(up_float)).astype(jnp.bfloat16)
    scaled = normed_back.astype(jnp.float32) * norm_gain
    gated_grad = inverse_std * (scaled - lax.optimization_barrier(jnp.mean(scaled, axis=-1, keepdims=True)) - normed * lax.optimization_barrier(jnp.mean(scaled * normed, axis=-1, keepdims=True)))
    gate_pre_grad = (gated_grad * gelu_slope(gate_float)).astype(jnp.bfloat16)
    flat_up = up_pre_grad.reshape(-1, GATED)
    flat_gate = gate_pre_grad.reshape(-1, GATED)
    flat_inputs = inputs.reshape(-1, MODEL)
    input_grad = jnp.dot(flat_up, up_weight.T, preferred_element_type=jnp.float32) + jnp.dot(flat_gate, gate_weight.T, preferred_element_type=jnp.float32)
    input_grad = input_grad.astype(jnp.bfloat16).reshape(BATCH, LENGTH, MODEL)
    up_weight_grad = jnp.dot(flat_inputs.T, flat_up, preferred_element_type=jnp.float32) * grad_scale
    gate_weight_grad = jnp.dot(flat_inputs.T, flat_gate, preferred_element_type=jnp.float32) * grad_scale
    return (input_grad, up_weight_grad, gate_weight_grad)
```

```python
import math

import jax
import jax.numpy as jnp
from jax import lax
from jax.experimental import pallas as pl
from jax.experimental.pallas import tpu as pltpu
from jax.sharding import PartitionSpec as P

MESH = pl.DeviceIdType.MESH
NX, NY, NZ = 4, 4, 8
ROWS = 256
GATED = 1024
MODEL = 2048
NG = 8
CH = 128
SEG = 64
f32, bf16 = jnp.float32, jnp.bfloat16

norm_eps = 1e-05
grad_scale = 1.0 / 256.0
root_half = 1.0 / math.sqrt(2.0)
root_twopi = 1.0 / math.sqrt(2.0 * math.pi)


def dot(a, b):
    return jnp.dot(a, b, preferred_element_type=f32)


def dot_t(a, b):
    return lax.dot_general(a, b, (((1,), (1,)), ((), ())), preferred_element_type=f32)


class Names:
    def __init__(self):
        self.at = {}

    def __call__(self, *key):
        return self.at.setdefault(key, len(self.at))


N_REMOTE = 160
N_LOCAL = 16


def kernel(
    x_hbm, up_hbm, gate_hbm, cot_hbm, gain_hbm, wu_hbm, wg_hbm, mix_hbm,
    ig_out, du_out, dg_out,
    upv, gatev, cotv, gainv, xo, xp, xt, mixd, mixo, mixin, peer, acc, back, cs, nrm, si,
    gu, gg, wb, outv, uorg, urec, uredf, uredb, uy, uyf, uyb, ux, agu,
    gorg, grec, gredf, gredb, gy, gyf, gyb, gz, agg, duv, dgv,
    send_sem, recv_sem, loc_sem,
):
    sp, dp = lax.axis_index("sp"), lax.axis_index("dp")
    z, x = sp // NX, sp % NX
    y, c = dp // 2, dp % 2
    h = x % 2

    def dev(dz=0, dx=0, dy=0, other=False):
        zz, xx, yy = (z + dz + NZ) % NZ, (x + dx + NX) % NX, (y + dy + NY) % NY
        cc = 1 - c if other else c
        return {"sp": zz * NX + xx, "dp": yy * 2 + cc}

    pair_dev = {"sp": z * NX + (x + 1 - 2 * h), "dp": dp}
    names, started = Names(), []

    def remote(key, src, dst, to):
        i = names(*key)
        return pltpu.make_async_remote_copy(
            src_ref=src, dst_ref=dst, send_sem=send_sem.at[i], recv_sem=recv_sem.at[i],
            device_id=to, device_id_type=MESH,
        )

    def send(key, src, dst, to):
        copy = remote(key, src, dst, to)
        copy.start()
        started.append(copy)

    def arrive(key, dst):
        remote(key, dst, dst, pair_dev).wait_recv()

    loads = {}

    def load(name, src, dst):
        copy = pltpu.make_async_copy(src, dst, loc_sem.at[len(loads)])
        copy.start()
        loads[name] = copy

    load("gate", gate_hbm.at[0], gatev)
    load("up", up_hbm.at[0], upv)
    load("cot", cot_hbm.at[0], cotv)
    load("gain", gain_hbm, gainv)
    off = pl.multiple_of(h * ROWS, ROWS)
    load("mixd", mix_hbm.at[:, pl.ds(off, ROWS), pl.ds(off, ROWS)], mixd)
    load("mixo", mix_hbm.at[:, pl.ds(ROWS, ROWS), pl.ds(0, ROWS)], mixo)

    def columns(block):
        return pl.ds(pl.multiple_of(block * ROWS, ROWS), ROWS)

    for k in range(NY):
        load(("x", k), x_hbm.at[0, :, columns(2 * k + c)], xo.at[k])
    load("wu", wu_hbm, wb.at[dp, 0])
    load("wg", wg_hbm, wb.at[dp, 1])

    peers = [dev(other=True)]
    peers += [dev(dy=k) for k in range(1, NY)]
    peers += [dev(dx=k) for k in range(1, NX)]
    peers += [dev(dz=k) for k in range(1, NZ)]
    barrier = pltpu.get_barrier_semaphore()
    for p in peers:
        pl.semaphore_signal(barrier, inc=1, device_id=p, device_id_type=MESH)
    pl.semaphore_wait(barrier, len(peers))

    up_w, gate_w = wu_hbm, wg_hbm
    mine = {0: up_w, 1: gate_w}
    for d, order in ((1, (0, 1)), (-1, (1, 0))):
        for part in order:
            send(("w", d, part), mine[part], wb.at[dp, part], dev(dy=d))
    for k in range(NY):
        send(("xp", k), x_hbm.at[0, :, columns(2 * k + 1 - c)], xp.at[k], dev(other=True))
    for part in range(2):
        send(("wc", 0, part), mine[part], wb.at[dp, part], dev(other=True))

    def block_of(dy, other=False):
        return ((y + dy + NY) % NY) * 2 + (1 - c if other else c)

    def weights_first():
        for d, part in ((1, 0), (-1, 1)):
            b = block_of(-d)
            arrive(("w", d, part), wb.at[b, part])
            send(("wf", d), wb.at[b, part], wb.at[b, part], dev(dy=d))
            send(("wc", -d, part), wb.at[b, part], wb.at[b, part], dev(other=True))

    def weights_second():
        for d, part in ((1, 1), (-1, 0)):
            b = block_of(-d)
            arrive(("w", d, part), wb.at[b, part])
            send(("wc", -d, part), wb.at[b, part], wb.at[b, part], dev(other=True))

    def weights_third():
        b = block_of(2)
        for d, part in ((1, 0), (-1, 1)):
            arrive(("wf", d), wb.at[b, part])
            send(("wc", 2, part), wb.at[b, part], wb.at[b, part], dev(other=True))

    def weights_other(dy):
        b = block_of(dy, True)
        for part in range(2):
            arrive(("wc", dy, part), wb.at[b, part])

    RB = 16
    for name in ("gate", "up", "cot", "gain"):
        loads[name].wait()

    def gate_rows(i, _):
        rows = pl.ds(pl.multiple_of(i * RB, RB), RB)
        a = gatev[rows, :].astype(f32)
        cdf = 0.5 * (1.0 + lax.erf(a * root_half))
        act = a * cdf
        centered = act - jnp.mean(act, axis=-1, keepdims=True)
        inv = lax.rsqrt(jnp.mean(centered * centered, axis=-1, keepdims=True) + norm_eps)
        normed = centered * inv
        nrm[rows, :] = normed
        si[rows, :] = inv * (cdf + a * jnp.exp(-0.5 * a * a) * root_twopi)
        value = (normed * gainv[...]).astype(bf16)
        for g in range(NG):
            mixin[0, g, rows, :] = value[:, g * CH : (g + 1) * CH]
        return 0

    def up_rows(i, _):
        rows = pl.ds(pl.multiple_of(i * RB, RB), RB)
        a = upv[rows, :].astype(f32)
        ct = cotv[rows, :].astype(f32)
        cdf = 0.5 * (1.0 + lax.erf(a * root_half))
        value = (ct * (a * cdf)).astype(bf16)
        slope = ct * (cdf + a * jnp.exp(-0.5 * a * a) * root_twopi)
        for g in range(NG):
            mixin[1, g, rows, :] = value[:, g * CH : (g + 1) * CH]
            cs[g, rows, :] = slope[:, g * CH : (g + 1) * CH]
        return 0

    lax.fori_loop(0, ROWS // RB, gate_rows, 0)
    lax.fori_loop(0, ROWS // RB, up_rows, 0)
    for g in range(NG):
        send(("pair", g), mixin.at[h, g], peer.at[g], pair_dev)

    loads["mixd"].wait()
    loads["mixo"].wait()
    seg_t = lax.broadcasted_iota(jnp.int32, (ROWS, ROWS), 0) // SEG
    seg_s = lax.broadcasted_iota(jnp.int32, (ROWS, ROWS), 1) // SEG
    keep = seg_s <= seg_t

    def diag(g):
        return jnp.where(keep, mixd[g].astype(f32), 0.0)

    def up_grad(g, spatial):
        gu[g, 0:ROWS, :] = (spatial.astype(bf16).astype(f32) * cs[g]).astype(bf16)

    def gate_grads():
        def rows_of(i, _):
            rows = pl.ds(pl.multiple_of(i * RB, RB), RB)
            nb = jnp.concatenate([back[g, rows, :] for g in range(NG)], axis=1)
            scaled = nb.astype(f32) * gainv[...]
            normed = nrm[rows, :]
            m1 = jnp.mean(scaled, axis=-1, keepdims=True)
            m2 = jnp.mean(scaled * normed, axis=-1, keepdims=True)
            grad = ((scaled - m1 - normed * m2) * si[rows, :]).astype(bf16)
            for k in range(NX):
                gg[k, rows, :] = grad[:, k * 256 : (k + 1) * 256]
            return 0

        lax.fori_loop(0, ROWS // RB, rows_of, 0)

    @pl.when(h == 0)
    def _():
        def step(g, _):
            d = diag(g)
            up_grad(g, dot(d.astype(bf16), mixin[0, g]))
            acc[g] = dot(d.T.astype(bf16), mixin[1, g])
            return 0

        lax.fori_loop(0, NG, step, 0)

    @pl.when(h == 1)
    def _():
        def step(g, _):
            d = diag(g)
            back[g] = dot(d.T.astype(bf16), mixin[1, g]).astype(bf16)
            acc[g] = dot(d.astype(bf16), mixin[0, g])
            return 0

        lax.fori_loop(0, NG, step, 0)
        gate_grads()

    for k in range(NY):
        loads[("x", k)].wait()
        xt[k, :, 0:ROWS] = xo[k].T
        arrive(("xp", k), xp.at[k])
        xt[k, :, ROWS : 2 * ROWS] = xp[k].T

    for g in range(NG):
        arrive(("pair", g), peer.at[g])

        @pl.when(h == 0)
        def _():
            back[g] = (acc[g] + dot(mixo[g].astype(f32).T.astype(bf16), peer[g])).astype(bf16)

        @pl.when(h == 1)
        def _():
            up_grad(g, acc[g] + dot(mixo[g], peer[g]))

    @pl.when(h == 0)
    def _():
        gate_grads()

    own, theirs = pl.ds(0, ROWS), pl.ds(ROWS, ROWS)
    send(("gu",), gu.at[:, own, :], gu.at[:, theirs, :], dev(other=True))
    send(("gg",), gg.at[:, own, :], gg.at[:, theirs, :], dev(other=True))
    arrive(("gu",), gu.at[:, theirs, :])
    arrive(("gg",), gg.at[:, theirs, :])

    def u_term(k, j):
        return dot(xt[k], gu[j])

    def g_term(k, j):
        return dot(xt[k], gg[j])

    def halves(d):
        long = 0 if d == 1 else 1
        return long, 1 - long

    def zi(v):
        return (z + v + NZ) % NZ

    def xi(v):
        return (x + v + NX) % NX

    di = {1: 0, -1: 1}

    def fill(dst, slot, term, half, j, add=None):
        for r in range(2):
            t = term(2 * half + r, j)
            if add is not None:
                t = t + add[slot, r].astype(f32)
            dst[slot, r] = t.astype(bf16)

    USLOT = {("L", k): k for k in range(4)} | {("S", k): 4 + k for k in range(3)}
    GSLOT = {("L", k): k for k in range(2)} | {("S", 0): 2}

    def u_slot(d, kind, k):
        return di[d] * 7 + USLOT[kind, k]

    def g_slot(d, kind, k):
        return di[d] * 3 + GSLOT[kind, k]

    def u_start():
        for kind, dist in (("L", 4), ("S", 3)):
            for d in (1, -1):
                half = halves(d)[0 if kind == "L" else 1]
                slot = di[d] * 2 + (0 if kind == "L" else 1)
                fill(uorg, slot, u_term, half, zi(d * dist))
                send(("u", d, kind, dist - 1), uorg.at[slot], urec.at[u_slot(d, kind, dist - 1)], dev(dz=d))

    def u_step(kind, k):
        for d in (1, -1):
            half = halves(d)[0 if kind == "L" else 1]
            slot = u_slot(d, kind, k)
            arrive(("u", d, kind, k), urec.at[slot])
            fill(urec, slot, u_term, half, zi(d * k), add=urec)
            send(("u", d, kind, k - 1), urec.at[slot], urec.at[u_slot(d, kind, k - 1)], dev(dz=d))

    def g_start():
        for kind, dist in (("L", 2), ("S", 1)):
            for d in (1, -1):
                half = halves(d)[0 if kind == "L" else 1]
                slot = di[d] * 2 + (0 if kind == "L" else 1)
                fill(gorg, slot, g_term, half, xi(d * dist))
                send(("g", d, kind, dist - 1), gorg.at[slot], grec.at[g_slot(d, kind, dist - 1)], dev(dx=d))

    def g_step(kind, k):
        for d in (1, -1):
            half = halves(d)[0 if kind == "L" else 1]
            slot = g_slot(d, kind, k)
            arrive(("g", d, kind, k), grec.at[slot])
            fill(grec, slot, g_term, half, xi(d * k), add=grec)
            send(("g", d, kind, k - 1), grec.at[slot], grec.at[g_slot(d, kind, k - 1)], dev(dx=d))

    def u_end():
        for d, kind in ((1, "S"), (-1, "S"), (1, "L"), (-1, "L")):
            arrive(("u", d, kind, 0), urec.at[u_slot(d, kind, 0)])
        for half in range(2):
            plus = u_slot(1, "L" if half == 0 else "S", 0)
            minus = u_slot(-1, "L" if half == 1 else "S", 0)
            for r in range(2):
                k = 2 * half + r
                t = u_term(k, z) + urec[plus, r].astype(f32) + urec[minus, r].astype(f32)
                uredf[k] = t
                uredb[k] = t.astype(bf16)
        for k in range(1, NY):
            to = (y + k) % NY
            send(("uy", k), uredb.at[to], uy.at[k - 1], dev(dy=k))

    def g_end():
        for d, kind in ((1, "S"), (-1, "S"), (1, "L"), (-1, "L")):
            arrive(("g", d, kind, 0), grec.at[g_slot(d, kind, 0)])
        for half in range(2):
            plus = g_slot(1, "L" if half == 0 else "S", 0)
            minus = g_slot(-1, "L" if half == 1 else "S", 0)
            for r in range(2):
                k = 2 * half + r
                t = g_term(k, x) + grec[plus, r].astype(f32) + grec[minus, r].astype(f32)
                gredf[k] = t
                gredb[k] = t.astype(bf16)
        for k in range(1, NY):
            to = (y + k) % NY
            send(("gy", k), gredb.at[to], gy.at[k - 1], dev(dy=k))

    def u_y():
        for k in range(1, NY):
            arrive(("uy", k), uy.at[k - 1])
        t = uredf[y]
        for k in range(1, NY):
            t = t + uy[k - 1].astype(f32)
        for k in range(NX):
            piece = t[k * 64 : (k + 1) * 64, :]
            uyf[k] = piece
            uyb[k] = piece.astype(bf16)
        for k in range(1, NX):
            send(("ux", k), uyb.at[xi(k)], ux.at[k - 1], dev(dx=k))

    def u_x():
        for k in range(1, NX):
            arrive(("ux", k), ux.at[k - 1])
        t = uyf[x]
        for k in range(1, NX):
            t = t + ux[k - 1].astype(f32)
        agu[x, z] = (t * grad_scale).astype(bf16)
        for k in range(1, NZ):
            send(("au", k), agu.at[x, z], agu.at[x, z], dev(dz=k))

    def g_y():
        for k in range(1, NY):
            arrive(("gy", k), gy.at[k - 1])
        t = gredf[y]
        for k in range(1, NY):
            t = t + gy[k - 1].astype(f32)
        for k in range(NZ):
            piece = t[k * 32 : (k + 1) * 32, :]
            gyf[k] = piece
            gyb[k] = piece.astype(bf16)
        for k in range(1, NZ):
            send(("gz", k), gyb.at[zi(k)], gz.at[k - 1], dev(dz=k))

    def g_z():
        for k in range(1, NZ):
            arrive(("gz", k), gz.at[k - 1])
        t = gyf[z]
        for k in range(1, NZ):
            t = t + gz[k - 1].astype(f32)
        agg[x, z] = (t * grad_scale).astype(bf16)
        for k in range(1, NZ):
            send(("ag", k), agg.at[x, z], agg.at[x, z], dev(dz=k))

    def gather_z(tag, buf):
        for k in range(1, NZ):
            arrive((tag, k), buf.at[x, zi(-k)])
        for d in (1, -1):
            send((tag, "x", d), buf.at[x], buf.at[x], dev(dx=d))

    def part_of(d):
        return pl.ds(0, NZ // 2) if d == 1 else pl.ds(NZ // 2, NZ // 2)

    def gather_x(tag, buf):
        for d in (1, -1):
            arrive((tag, "x", d), buf.at[xi(-d)])
            send((tag, "xx", d), buf.at[xi(-d), part_of(d)], buf.at[xi(-d), part_of(d)], dev(dx=d))

    def gather_last(tag, buf):
        for d in (1, -1):
            arrive((tag, "xx", d), buf.at[xi(2), part_of(d)])

    def out_block(b):
        lu = jnp.concatenate([gu[g, 0:ROWS, :] for g in range(NG)], axis=1)
        lg = jnp.concatenate([gg[g, 0:ROWS, :] for g in range(NX)], axis=1)
        t = dot_t(lu, wb[b, 0]) + dot_t(lg, wb[b, 1])
        outv[b] = t.astype(bf16)

    stores = []

    def store_block(b, i):
        copy = pltpu.make_async_copy(outv.at[b], ig_out.at[:, columns(b)], loc_sem.at[i])
        copy.start()
        stores.append(copy)

    u_start()
    g_start()
    weights_first()
    u_step("L", 3)
    g_step("L", 1)
    u_step("S", 2)
    u_step("L", 2)
    loads["wu"].wait()
    loads["wg"].wait()
    weights_second()
    u_step("S", 1)
    u_step("L", 1)
    g_end()
    u_end()
    out_block(block_of(0))
    weights_third()
    u_y()
    g_y()
    weights_other(0)
    out_block(block_of(0, True))
    out_block(block_of(1))
    u_x()
    g_z()
    out_block(block_of(3))
    gather_z("au", agu)
    gather_z("ag", agg)
    out_block(block_of(2))
    weights_other(1)
    out_block(block_of(1, True))
    gather_x("au", agu)
    gather_x("ag", agg)
    weights_other(-1)
    out_block(block_of(3, True))
    weights_other(2)
    out_block(block_of(2, True))
    for b in range(8):
        store_block(b, b)
    gather_last("au", agu)
    for i in range(NX):
        for j in range(NZ):
            duv[i * 64 : (i + 1) * 64, j * CH : (j + 1) * CH] = agu[i, j].astype(f32)
    copy = pltpu.make_async_copy(duv, du_out, loc_sem.at[8])
    copy.start()
    stores.append(copy)
    gather_last("ag", agg)
    for i in range(NX):
        for j in range(NZ):
            dgv[j * 32 : (j + 1) * 32, i * 256 : (i + 1) * 256] = agg[i, j].astype(f32)
    copy = pltpu.make_async_copy(dgv, dg_out, loc_sem.at[9])
    copy.start()
    stores.append(copy)
    for copy in started:
        copy.wait_send()
    for copy in stores:
        copy.wait()
    assert len(names.at) <= N_REMOTE and len(loads) <= N_LOCAL


def on_device(inputs, up_pre, gate_pre, cotangent, norm_gain, up_weight, gate_weight, mix_weight):
    V = pltpu.VMEM
    scratch = [
        V((ROWS, GATED), bf16), V((ROWS, GATED), bf16), V((ROWS, GATED), bf16), V((1, GATED), f32),
        V((NY, ROWS, ROWS), bf16), V((NY, ROWS, ROWS), bf16), V((NY, ROWS, 2 * ROWS), bf16),
        V((NG, ROWS, ROWS), bf16), V((NG, ROWS, ROWS), bf16),
        V((2, NG, ROWS, CH), bf16), V((NG, ROWS, CH), bf16), V((NG, ROWS, CH), f32), V((NG, ROWS, CH), bf16),
        V((NG, ROWS, CH), f32), V((ROWS, GATED), f32), V((ROWS, GATED), f32),
        V((NG, 2 * ROWS, CH), bf16), V((NX, 2 * ROWS, 256), bf16),
        V((8, 2, ROWS, GATED), bf16), V((8, ROWS, ROWS), bf16),
        V((4, 2, ROWS, CH), bf16), V((14, 2, ROWS, CH), bf16),
        V((NY, ROWS, CH), f32), V((NY, ROWS, CH), bf16), V((3, ROWS, CH), bf16),
        V((NX, 64, CH), f32), V((NX, 64, CH), bf16), V((3, 64, CH), bf16), V((NX, NZ, 64, CH), bf16),
        V((4, 2, ROWS, 256), bf16), V((6, 2, ROWS, 256), bf16),
        V((NY, ROWS, 256), f32), V((NY, ROWS, 256), bf16), V((3, ROWS, 256), bf16),
        V((NZ, 32, 256), f32), V((NZ, 32, 256), bf16), V((7, 32, 256), bf16), V((NX, NZ, 32, 256), bf16),
        V((ROWS, GATED), f32), V((ROWS, GATED), f32),
        pltpu.SemaphoreType.DMA((N_REMOTE,)), pltpu.SemaphoreType.DMA((N_REMOTE,)),
        pltpu.SemaphoreType.DMA((N_LOCAL,)),
    ]
    anywhere = pl.BlockSpec(memory_space=pl.ANY)
    input_grad, up_grad, gate_grad = pl.pallas_call(
        kernel,
        out_shape=(
            jax.ShapeDtypeStruct((ROWS, MODEL), bf16),
            jax.ShapeDtypeStruct((ROWS, GATED), f32),
            jax.ShapeDtypeStruct((ROWS, GATED), f32),
        ),
        in_specs=[anywhere] * 8,
        out_specs=(anywhere,) * 3,
        scratch_shapes=scratch,
        compiler_params=pltpu.CompilerParams(
            collective_id=0, has_side_effects=True, vmem_limit_bytes=60 * 1024 * 1024
        ),
    )(
        inputs, up_pre, gate_pre, cotangent, norm_gain.reshape(1, GATED), up_weight, gate_weight, mix_weight,
    )
    return input_grad[None], up_grad, gate_grad


def solution(mesh):
    return jax.shard_map(
        on_device,
        mesh=mesh,
        in_specs=(
            P("dp", "sp", None),
            P("dp", "sp", None),
            P("dp", "sp", None),
            P("dp", "sp", None),
            P(),
            P("dp", None),
            P("dp", None),
            P(),
        ),
        out_specs=(P("dp", "sp", None), P("dp", None), P("dp", None)),
        check_vma=False,
    )
```

```python
import math

import jax
import jax.numpy as jnp
from jax import lax
from jax.experimental import pallas as pl
from jax.experimental.pallas import tpu as pltpu
from jax.sharding import PartitionSpec as P

MESH = pl.DeviceIdType.MESH
NX, NY, NZ = 4, 4, 8
ROWS = 256
GATED = 1024
MODEL = 2048
NG = 8
CH = 128
SEG = 64
RB = 16
f32, bf16 = jnp.float32, jnp.bfloat16

norm_eps = 1e-05
grad_scale = 1.0 / 256.0
root_half = 1.0 / math.sqrt(2.0)
root_twopi = 1.0 / math.sqrt(2.0 * math.pi)


def dot(a, b):
    return jnp.dot(a, b, preferred_element_type=f32)


def dot_t(a, b):
    return lax.dot_general(a, b, (((1,), (1,)), ((), ())), preferred_element_type=f32)


class Names:
    def __init__(self):
        self.at = {}

    def __call__(self, *key):
        return self.at.setdefault(key, len(self.at))


N_SEND = 18
N_RECV = 71
N_LOCAL = 7


def kernel(
    x_hbm, up_hbm, gate_hbm, cot_hbm, gainv, wu_hbm, wg_hbm, mix_hbm,
    ig_out, du_out, dg_out,
    upv, gatev, cotv, xo, xp, xt, mixd, mixo, mixin, peer, acc, back, cs, nrm, si,
    gu, gg, wb, uorg, urec, gorg, grec, redf, redb, yrec, subf, subb, ux, gz, agu, agg,
    send_sem, recv_sem, loc_sem,
):
    sp, dp = lax.axis_index("sp"), lax.axis_index("dp")
    z, x = sp // NX, sp % NX
    y, c = dp // 2, dp % 2
    h = x % 2

    def dev(dz=0, dx=0, dy=0, other=False):
        zz, xx, yy = (z + dz + NZ) % NZ, (x + dx + NX) % NX, (y + dy + NY) % NY
        cc = 1 - c if other else c
        return {"sp": zz * NX + xx, "dp": yy * 2 + cc}

    def zi(v):
        return (z + v + NZ) % NZ

    def xi(v):
        return (x + v + NX) % NX

    def yi(v):
        return (y + v + NY) % NY

    pair_dev = {"sp": z * NX + (x + 1 - 2 * h), "dp": dp}
    families, names, held = Names(), Names(), {}

    def bytes_of(ref):
        return math.prod(ref.shape) * ref.dtype.itemsize

    def remote(family, key, src, dst, to):
        return pltpu.make_async_remote_copy(
            src_ref=src, dst_ref=dst, send_sem=send_sem.at[families(family)], recv_sem=recv_sem.at[names(*key)],
            device_id=to, device_id_type=MESH,
        )

    def send(family, key, src, dst, to, note=True):
        remote(family, key, src, dst, to).start()
        if note:
            held[family] = held.get(family, 0) + bytes_of(src)

    def arrive(key, dst):
        pltpu.make_async_copy(dst, dst, recv_sem.at[names(*key)]).wait()

    def all_sent(family, ref):
        assert held.pop(family) == bytes_of(ref), family
        pltpu.make_async_copy(ref, ref, send_sem.at[families(family)]).wait()

    peers = [dev(other=True)]
    peers += [dev(dy=k) for k in range(1, NY)]
    peers += [dev(dx=k) for k in range(1, NX)]
    peers += [dev(dz=k) for k in range(1, NZ)]
    barrier = pltpu.get_barrier_semaphore()
    for p in peers:
        pl.semaphore_signal(barrier, inc=1, device_id=p, device_id_type=MESH)

    local = Names()

    def load(name, src, dst):
        pltpu.make_async_copy(src, dst, loc_sem.at[local(name)]).start()

    def loaded(name, ref):
        pltpu.make_async_copy(ref, ref, loc_sem.at[local(name)]).wait()

    load("gate", gate_hbm.at[0], gatev)
    load("up", up_hbm.at[0], upv)
    load("cot", cot_hbm.at[0], cotv)
    off = pl.multiple_of(h * ROWS, ROWS)
    load("mixd", mix_hbm.at[:, pl.ds(off, ROWS), pl.ds(off, ROWS)], mixd)
    load("mixo", mix_hbm.at[:, pl.ds(ROWS, ROWS), pl.ds(0, ROWS)], mixo)

    def columns(block):
        return pl.ds(pl.multiple_of(block * ROWS, ROWS), ROWS)

    for k in range(NY):
        load("x", x_hbm.at[0, :, columns(2 * k + c)], xo.at[k])
    load("w", wu_hbm, wb.at[dp, 0])
    load("w", wg_hbm, wb.at[dp, 1])

    def gate_rows(i, _):
        rows = pl.ds(pl.multiple_of(i * RB, RB), RB)
        a = gatev[rows, :].astype(f32)
        cdf = 0.5 * (1.0 + lax.erf(a * root_half))
        act = a * cdf
        centered = act - jnp.mean(act, axis=-1, keepdims=True)
        inv = lax.rsqrt(jnp.mean(centered * centered, axis=-1, keepdims=True) + norm_eps)
        normed = centered * inv
        nrm[rows, :] = normed
        si[rows, :] = inv * (cdf + a * jnp.exp(-0.5 * a * a) * root_twopi)
        value = (normed * gainv[...]).astype(bf16)
        for g in range(NG):
            mixin[0, g, rows, :] = value[:, g * CH : (g + 1) * CH]
        return 0

    def up_rows(i, _):
        rows = pl.ds(pl.multiple_of(i * RB, RB), RB)
        a = upv[rows, :].astype(f32)
        ct = cotv[rows, :].astype(f32)
        cdf = 0.5 * (1.0 + lax.erf(a * root_half))
        value = (ct * (a * cdf)).astype(bf16)
        slope = ct * (cdf + a * jnp.exp(-0.5 * a * a) * root_twopi)
        for g in range(NG):
            mixin[1, g, rows, :] = value[:, g * CH : (g + 1) * CH]
            cs[g, rows, :] = slope[:, g * CH : (g + 1) * CH]
        return 0

    loaded("gate", gatev)
    lax.fori_loop(0, ROWS // RB, gate_rows, 0, unroll=4)
    loaded("up", upv)
    loaded("cot", cotv)
    lax.fori_loop(0, ROWS // RB, up_rows, 0)
    pl.semaphore_wait(barrier, len(peers))

    order = [zi(v) for v in (4, 3, -3, 2, -2, 1, -1, 0)]
    for j, g in enumerate(order):
        send("pair", ("pair", j), mixin.at[h, g], peer.at[j], pair_dev)

    mine = {0: wu_hbm, 1: wg_hbm}
    for d, parts in ((1, (0, 1)), (-1, (1, 0))):
        for part in parts:
            send("w", ("w", d, part), mine[part], wb.at[dp, part], dev(dy=d))
    for k in range(NY):
        send("xp", ("xp",), x_hbm.at[0, :, columns(2 * k + 1 - c)], xp.at[k], dev(other=True))

    def block_of(dy, other=False):
        return yi(dy) * 2 + (1 - c if other else c)

    def weights_own():
        for part in range(2):
            send("wc", ("wc", 0), mine[part], wb.at[dp, part], dev(other=True))

    def weights_first():
        for d, part in ((1, 0), (-1, 1)):
            b = block_of(-d)
            arrive(("w", d, part), wb.at[b, part])
            send("wc", ("wc", -d), wb.at[b, part], wb.at[b, part], dev(other=True))

    def weights_pass(f):
        rows = pl.ds(f * 64, 64)
        for d, part in ((1, 0), (-1, 1)):
            b = block_of(-d)
            send("wf", ("wf", f), wb.at[b, part, rows], wb.at[b, part, rows], dev(dy=d))

    def weights_second():
        for d, part in ((1, 1), (-1, 0)):
            b = block_of(-d)
            arrive(("w", d, part), wb.at[b, part])
            send("wc", ("wc", -d), wb.at[b, part], wb.at[b, part], dev(other=True))

    def weights_third(f):
        b, rows = block_of(2), pl.ds(f * 64, 64)
        arrive(("wf", f), wb.at[b, :, rows])
        send("wc", ("wc", 2), wb.at[b, :, rows], wb.at[b, :, rows], dev(other=True))

    def weights_other(dy):
        b = block_of(dy, True)
        arrive(("wc", dy), wb.at[b])

    own, theirs = pl.ds(0, ROWS), pl.ds(ROWS, ROWS)
    loaded("mixd", mixd)
    loaded("mixo", mixo)
    seg_t = lax.broadcasted_iota(jnp.int32, (ROWS, ROWS), 0) // SEG
    seg_s = lax.broadcasted_iota(jnp.int32, (ROWS, ROWS), 1) // SEG
    keep = seg_s <= seg_t

    def diag(g):
        return jnp.where(keep, mixd[g].astype(f32), 0.0)

    def up_grad(g, spatial):
        gu[g, 0:ROWS, :] = (spatial.astype(bf16).astype(f32) * cs[g]).astype(bf16)

    def share_up(j):
        g = order[j]
        send("gu", ("gu", j), gu.at[g, own], gu.at[g, theirs], dev(other=True), note=False)

    def up_here(j):
        g = order[j]
        arrive(("gu", j), gu.at[g, theirs])

    def gate_grads():
        def rows_of(i, _):
            rows = pl.ds(pl.multiple_of(i * RB, RB), RB)
            nb = jnp.concatenate([back[g, rows, :] for g in range(NG)], axis=1)
            scaled = nb.astype(f32) * gainv[...]
            normed = nrm[rows, :]
            m1 = jnp.mean(scaled, axis=-1, keepdims=True)
            m2 = jnp.mean(scaled * normed, axis=-1, keepdims=True)
            grad = ((scaled - m1 - normed * m2) * si[rows, :]).astype(bf16)
            for g in range(NG):
                gg[g, rows, :] = grad[:, g * CH : (g + 1) * CH]
            return 0

        lax.fori_loop(0, ROWS // RB, rows_of, 0, unroll=4)
        send("gg", ("gg",), gg.at[:, own, :], gg.at[:, theirs, :], dev(other=True), note=False)

    @pl.when(h == 0)
    def _():
        def step(g, _):
            d = diag(g)
            up_grad(g, dot(d.astype(bf16), mixin[0, g]))
            acc[g] = dot(d.T.astype(bf16), mixin[1, g])
            return 0

        lax.fori_loop(0, NG, step, 0)
        for j in range(NG):
            share_up(j)

    @pl.when(h == 1)
    def _():
        def step(g, _):
            d = diag(g)
            back[g] = dot(d.T.astype(bf16), mixin[1, g]).astype(bf16)
            acc[g] = dot(d.astype(bf16), mixin[0, g])
            return 0

        lax.fori_loop(0, NG, step, 0)

    loaded("x", xo)
    arrive(("xp",), xp)
    for k in range(NY):
        xt[k, :, 0:ROWS] = xo[k].T
        xt[k, :, ROWS : 2 * ROWS] = xp[k].T

    def pair_step(j):
        g = order[j]
        arrive(("pair", j), peer.at[j])

        @pl.when(h == 0)
        def _():
            back[g] = (acc[g] + dot(mixo[g].astype(f32).T.astype(bf16), peer[j])).astype(bf16)

        @pl.when(h == 1)
        def _():
            up_grad(g, acc[g] + dot(mixo[g], peer[j]))
            share_up(j)

    def late_gate():
        @pl.when(h == 0)
        def _():
            gate_grads()

    def early_gate():
        @pl.when(h == 1)
        def _():
            gate_grads()

    def gate_here():
        arrive(("gg",), gg.at[:, theirs, :])

    def u_term(k, j):
        return dot(xt[k], gu[j])

    def g_term(s):
        return lambda k, j: dot(xt[k], gg[2 * j + s])

    def half_of(d, kind):
        long = 0 if d == 1 else 1
        return long if kind == "L" else 1 - long

    di = {1: 0, -1: 1}

    def fill(dst, slot, term, half, j, add=False):
        for r in range(2):
            t = term(2 * half + r, j)
            if add:
                t = t + dst[slot, r].astype(f32)
            dst[slot, r] = t.astype(bf16)

    def u_slot(d, kind, k):
        return di[d] * 7 + (k if kind == "L" else 4 + k)

    def chain_key(name, d, kind, k):
        return (name, d, kind, k) if k else (name, 0)

    def u_start(kind, dist, directions=(1, -1)):
        for d in directions:
            slot = di[d] * 2 + (0 if kind == "L" else 1)
            fill(uorg, slot, u_term, half_of(d, kind), zi(d * dist))
            send("u", chain_key("u", d, kind, dist - 1), uorg.at[slot], urec.at[u_slot(d, kind, dist - 1)], dev(dz=d))

    def u_step(kind, k):
        for d in (1, -1):
            slot = u_slot(d, kind, k)
            arrive(("u", d, kind, k), urec.at[slot])
            fill(urec, slot, u_term, half_of(d, kind), zi(d * k), add=True)
            send("u", chain_key("u", d, kind, k - 1), urec.at[slot], urec.at[u_slot(d, kind, k - 1)], dev(dz=d))

    def g_slot(s, d, kind, k):
        return s * 6 + di[d] * 3 + (k if kind == "L" else 2)

    def g_start(s, kind, dist):
        for d in (1, -1):
            slot = s * 4 + di[d] * 2 + (0 if kind == "L" else 1)
            fill(gorg, slot, g_term(s), half_of(d, kind), xi(d * dist))
            send("g", chain_key(("g", s), d, kind, dist - 1), gorg.at[slot], grec.at[g_slot(s, d, kind, dist - 1)], dev(dx=d))

    def g_step(s):
        for d in (1, -1):
            slot = g_slot(s, d, "L", 1)
            arrive(chain_key(("g", s), d, "L", 1), grec.at[slot])
            fill(grec, slot, g_term(s), half_of(d, "L"), xi(d), add=True)
            send("g", chain_key(("g", s), d, "L", 0), grec.at[slot], grec.at[g_slot(s, d, "L", 0)], dev(dx=d))

    def y_slot(d, kind, k):
        return di[d] * 3 + (k if kind == "L" else 2)

    def y_rows(d, kind):
        return pl.ds(half_of(d, kind) * 128, 128)

    def close(s, rec, slot_of, key, term, j):
        arrive(key, rec.at[pl.ds(0, 4)])
        for half in range(2):
            plus = slot_of(1, "L" if half == 0 else "S")
            minus = slot_of(-1, "L" if half == 1 else "S")
            for r in range(2):
                k = 2 * half + r
                t = term(k, j) + rec[plus, r].astype(f32) + rec[minus, r].astype(f32)
                redf[s, k] = t
                redb[s, k] = t.astype(bf16)
        for kind, dist in (("L", 2), ("S", 1)):
            for d in (1, -1):
                rows = y_rows(d, kind)
                send("y", chain_key(("y", s), d, kind, dist - 1), redb.at[s, yi(d * dist), rows], yrec.at[s, y_slot(d, kind, dist - 1)], dev(dy=d))

    def u_end():
        close(2, urec, lambda d, kind: u_slot(d, kind, 0), ("u", 0), u_term, z)

    def g_end(s):
        close(s, grec, lambda d, kind: g_slot(s, d, kind, 0), (("g", s), 0), g_term(s), x)

    def y_step(s):
        for d in (1, -1):
            slot, rows = y_slot(d, "L", 1), y_rows(d, "L")
            arrive(chain_key(("y", s), d, "L", 1), yrec.at[s, slot])
            yrec[s, slot] = (yrec[s, slot].astype(f32) + redf[s, yi(d), rows, :]).astype(bf16)
            send("y", chain_key(("y", s), d, "L", 0), yrec.at[s, slot], yrec.at[s, y_slot(d, "L", 0)], dev(dy=d))

    def y_sum(s):
        arrive((("y", s), 0), yrec.at[s, pl.ds(0, 4)])
        for half in range(2):
            plus = y_slot(1, "L" if half == 0 else "S", 0)
            minus = y_slot(-1, "L" if half == 1 else "S", 0)
            rows = pl.ds(half * 128, 128)
            t = redf[s, y, rows, :] + yrec[s, plus].astype(f32) + yrec[s, minus].astype(f32)
            subf[s, rows, :] = t
            subb[s, rows, :] = t.astype(bf16)

    def rows64(v):
        return pl.ds(pl.multiple_of(v * 64, 64), 64)

    def rows32(v):
        return pl.ds(pl.multiple_of(v * 32, 32), 32)

    def y_end(s):
        y_sum(s)
        if s == 2:
            for k in range(1, NX):
                send("ux", ("ux",), subb.at[2, rows64(xi(k))], ux.at[k - 1], dev(dx=k))
        else:
            for k in range(1, NZ):
                send("gz", ("gz", s), subb.at[s, rows32(zi(k))], gz.at[s, k - 1], dev(dz=k))

    def piece_u():
        arrive(("ux",), ux)
        t = subf[2, rows64(x), :]
        for k in range(1, NX):
            t = t + ux[k - 1].astype(f32)
        agu[x, z] = t.astype(bf16)
        for k in range(1, NZ):
            send("au", ("a", 2), agu.at[x, z], agu.at[x, z], dev(dz=k))

    def piece_g(s):
        arrive(("gz", s), gz.at[s])
        t = subf[s, rows32(z), :]
        for k in range(1, NZ):
            t = t + gz[s, k - 1].astype(f32)
        agg[s, x, z] = t.astype(bf16)
        for k in range(1, NZ):
            send("ag", ("a", s), agg.at[s, x, z], agg.at[s, x, z], dev(dz=k))

    def gathered(s):
        return agu if s == 2 else agg.at[s]

    def gather_z(s):
        buf = gathered(s)
        arrive(("a", s), buf.at[0, pl.ds(0, NZ - 1)])
        for d in (1, -1):
            send("axu" if s == 2 else "axg", ("ax", s, d), buf.at[x], buf.at[x], dev(dx=d))

    def part_of(d):
        return pl.ds(0, NZ // 2) if d == 1 else pl.ds(NZ // 2, NZ // 2)

    def gather_x(s):
        buf = gathered(s)
        for d in (1, -1):
            arrive(("ax", s, d), buf.at[xi(-d)])
            send("axxu" if s == 2 else "axxg", ("axx", s), buf.at[xi(-d), part_of(d)], buf.at[xi(-d), part_of(d)], dev(dx=d))

    def gather_last(s):
        arrive(("axx", s), gathered(s).at[xi(2)])

    def out_block(b):
        lu = jnp.concatenate([gu[g, 0:ROWS, :] for g in range(NG)], axis=1)
        lg = jnp.concatenate([gg[g, 0:ROWS, :] for g in range(NG)], axis=1)
        ig_out[:, columns(b)] = (dot_t(lu, wb[b, 0]) + dot_t(lg, wb[b, 1])).astype(bf16)

    def put_up():
        for i in range(NX):
            for j in range(NZ):
                du_out[i * 64 : (i + 1) * 64, j * CH : (j + 1) * CH] = agu[i, j]

    def put_gate():
        for s in range(2):
            for i in range(NX):
                for j in range(NZ):
                    at = (2 * i + s) * CH
                    dg_out[j * 32 : (j + 1) * 32, at : at + CH] = agg[s, i, j]

    def finish_waits():
        held["gu"], held["gg"] = bytes_of(gu.at[:, own]), bytes_of(gg.at[:, own])
        for family, ref in (
            ("pair", mixin.at[0]), ("w", wb.at[pl.ds(0, 2)]), ("xp", xp), ("wc", wb.at[pl.ds(0, 4)]), ("wf", wb.at[0]),
            ("gu", gu.at[:, own]), ("gg", gg.at[:, own]), ("u", urec), ("g", grec), ("y", yrec), ("ux", ux), ("gz", gz),
            ("au", agu.at[0, pl.ds(0, NZ - 1)]), ("ag", agg.at[:, 0, pl.ds(0, NZ - 1)]),
            ("axu", agu.at[pl.ds(0, 2)]), ("axg", agg.at[:, pl.ds(0, 2)]), ("axxu", agu.at[0]), ("axxg", agg.at[:, 0]),
        ):
            all_sent(family, ref)
        assert not held

    pair_step(0)
    up_here(0)
    u_start("L", 4)
    pair_step(1)
    up_here(1)
    u_start("S", 3, (1,))
    pair_step(2)
    up_here(2)
    u_start("S", 3, (-1,))
    early_gate()
    weights_own()
    pair_step(3)
    pair_step(4)
    up_here(3)
    up_here(4)
    u_step("L", 3)
    pair_step(5)
    pair_step(6)
    pair_step(7)
    late_gate()
    gate_here()
    g_start(0, "L", 2)
    u_step("S", 2)
    g_start(0, "S", 1)
    g_start(1, "L", 2)
    up_here(5)
    up_here(6)
    up_here(7)
    u_step("L", 2)
    weights_first()
    weights_pass(0)
    g_step(0)
    g_start(1, "S", 1)
    u_step("S", 1)
    loaded("w", wb.at[dp])
    out_block(block_of(0))
    u_step("L", 1)
    weights_other(0)
    out_block(block_of(0, True))
    g_step(1)
    weights_second()
    g_end(0)
    u_end()
    out_block(block_of(1))
    y_step(0)
    y_step(2)
    g_end(1)
    y_end(0)
    y_end(2)
    weights_pass(1)
    out_block(block_of(3))
    y_step(1)
    weights_other(1)
    out_block(block_of(1, True))
    piece_g(0)
    y_end(1)
    weights_pass(2)
    weights_pass(3)
    piece_u()
    weights_other(-1)
    out_block(block_of(3, True))
    gather_z(0)
    piece_g(1)
    gather_z(2)
    weights_third(0)
    gather_x(0)
    weights_third(1)
    gather_z(1)
    gather_x(2)
    weights_third(2)
    gather_last(0)
    weights_third(3)
    gather_x(1)
    out_block(block_of(2))
    gather_last(2)
    put_up()
    weights_other(2)
    out_block(block_of(2, True))
    gather_last(1)
    put_gate()
    finish_waits()
    assert (len(families.at), len(names.at), len(local.at)) == (N_SEND, N_RECV, N_LOCAL), (len(families.at), len(names.at), len(local.at))


def on_device(inputs, up_pre, gate_pre, cotangent, norm_gain, up_weight, gate_weight, mix_weight):
    V = pltpu.VMEM
    scratch = [
        V((ROWS, GATED), bf16), V((ROWS, GATED), bf16), V((ROWS, GATED), bf16),
        V((NY, ROWS, ROWS), bf16), V((NY, ROWS, ROWS), bf16), V((NY, ROWS, 2 * ROWS), bf16),
        V((NG, ROWS, ROWS), bf16), V((NG, ROWS, ROWS), bf16),
        V((2, NG, ROWS, CH), bf16), V((NG, ROWS, CH), bf16), V((NG, ROWS, CH), f32), V((NG, ROWS, CH), bf16),
        V((NG, ROWS, CH), f32), V((ROWS, GATED), f32), V((ROWS, GATED), f32),
        V((NG, 2 * ROWS, CH), bf16), V((NG, 2 * ROWS, CH), bf16),
        V((8, 2, ROWS, GATED), bf16),
        V((4, 2, ROWS, CH), bf16), V((14, 2, ROWS, CH), bf16),
        V((8, 2, ROWS, CH), bf16), V((12, 2, ROWS, CH), bf16),
        V((3, NY, ROWS, CH), f32), V((3, NY, ROWS, CH), bf16), V((3, 6, 128, CH), bf16),
        V((3, ROWS, CH), f32), V((3, ROWS, CH), bf16),
        V((3, 64, CH), bf16), V((2, 7, 32, CH), bf16), V((NX, NZ, 64, CH), bf16), V((2, NX, NZ, 32, CH), bf16),
        pltpu.SemaphoreType.DMA((N_SEND,)), pltpu.SemaphoreType.DMA((N_RECV,)),
        pltpu.SemaphoreType.DMA((N_LOCAL,)),
    ]
    anywhere = pl.BlockSpec(memory_space=pl.ANY)
    inside = pl.BlockSpec(memory_space=pltpu.VMEM)
    input_grad, up_grad, gate_grad = pl.pallas_call(
        kernel,
        out_shape=(
            pltpu.VMEM((ROWS, MODEL), bf16),
            pltpu.VMEM((ROWS, GATED), bf16),
            pltpu.VMEM((ROWS, GATED), bf16),
        ),
        in_specs=[anywhere] * 4 + [inside] + [anywhere] * 3,
        out_specs=(inside,) * 3,
        scratch_shapes=scratch,
        compiler_params=pltpu.CompilerParams(
            collective_id=0, has_side_effects=True, vmem_limit_bytes=67043328 - 2097152 - 65536
        ),
    )(
        inputs, up_pre, gate_pre, cotangent, norm_gain.reshape(1, GATED), up_weight, gate_weight, mix_weight,
    )
    hbm = pl.BlockSpec(memory_space=pl.ANY)
    return pl.pallas_call(
        widen,
        out_shape=(
            jax.ShapeDtypeStruct((1, ROWS, MODEL), bf16),
            jax.ShapeDtypeStruct((ROWS, GATED), f32),
            jax.ShapeDtypeStruct((ROWS, GATED), f32),
        ),
        in_specs=[inside] * 3,
        out_specs=(hbm,) * 3,
        scratch_shapes=[V((ROWS, GATED), f32), V((ROWS, GATED), f32), pltpu.SemaphoreType.DMA((5,))],
        compiler_params=pltpu.CompilerParams(vmem_limit_bytes=8 * 1024 * 1024),
    )(input_grad, up_grad, gate_grad)


def widen(ig, du, dg, ig_out, du_out, dg_out, duw, dgw, sem):
    copies = [pltpu.make_async_copy(ig, ig_out.at[0], sem.at[0])]
    copies[0].start()
    half = ROWS // 2
    for k, (src, mid, dst) in enumerate(((du, duw, du_out), (dg, dgw, dg_out))):
        for r in range(2):
            rows = pl.ds(r * half, half)
            mid[rows, :] = src[rows, :].astype(f32) * grad_scale
            copies.append(pltpu.make_async_copy(mid.at[rows], dst.at[rows], sem.at[1 + 2 * k + r]))
            copies[-1].start()
    for copy in copies:
        copy.wait()


def solution(mesh):
    return jax.shard_map(
        on_device,
        mesh=mesh,
        in_specs=(
            P("dp", "sp", None),
            P("dp", "sp", None),
            P("dp", "sp", None),
            P("dp", "sp", None),
            P(),
            P("dp", None),
            P("dp", None),
            P(),
        ),
        out_specs=(P("dp", "sp", None), P("dp", None), P("dp", None)),
        check_vma=False,
    )
```

```python
import math

import jax
import jax.numpy as jnp
from jax import lax
from jax.experimental import pallas as pl
from jax.experimental.pallas import tpu as pltpu
from jax.sharding import PartitionSpec as P

MESH = pl.DeviceIdType.MESH
NX, NY, NZ = 4, 4, 8
ROWS = 256
GATED = 1024
MODEL = 2048
NG = 8
CH = 128
SEG = 64
RB = 16
f32, bf16 = jnp.float32, jnp.bfloat16

norm_eps = 1e-05
grad_scale = 1.0 / 256.0
root_half = 1.0 / math.sqrt(2.0)
root_twopi = 1.0 / math.sqrt(2.0 * math.pi)


def dot(a, b):
    return jnp.dot(a, b, preferred_element_type=f32)


def dot_t(a, b):
    return lax.dot_general(a, b, (((1,), (1,)), ((), ())), preferred_element_type=f32)


class Names:
    def __init__(self):
        self.at = {}

    def __call__(self, *key):
        return self.at.setdefault(key, len(self.at))


N_SEND = 18
N_RECV = 71
N_LOCAL = 7


def kernel(
    x_hbm, up_hbm, gate_hbm, cot_hbm, gainv, wu_hbm, wg_hbm, mix_hbm,
    ig_out, du_out, dg_out,
    upv, gatev, cotv, xo, xp, xt, mixd, mixo, mixin, peer, acc, back, cs, nrm, si,
    gu, gg, wb, uorg, urec, gorg, grec, redf, redb, yrec, subf, subb, ux, gz, agu, agg,
    send_sem, recv_sem, loc_sem,
):
    sp, dp = lax.axis_index("sp"), lax.axis_index("dp")
    z, x = sp // NX, sp % NX
    y, c = dp // 2, dp % 2
    h = x % 2

    def dev(dz=0, dx=0, dy=0, other=False):
        zz, xx, yy = (z + dz + NZ) % NZ, (x + dx + NX) % NX, (y + dy + NY) % NY
        cc = 1 - c if other else c
        return {"sp": zz * NX + xx, "dp": yy * 2 + cc}

    def zi(v):
        return (z + v + NZ) % NZ

    def xi(v):
        return (x + v + NX) % NX

    def yi(v):
        return (y + v + NY) % NY

    pair_dev = {"sp": z * NX + (x + 1 - 2 * h), "dp": dp}
    families, names, held = Names(), Names(), {}

    def bytes_of(ref):
        return math.prod(ref.shape) * ref.dtype.itemsize

    def remote(family, key, src, dst, to):
        return pltpu.make_async_remote_copy(
            src_ref=src, dst_ref=dst, send_sem=send_sem.at[families(family)], recv_sem=recv_sem.at[names(*key)],
            device_id=to, device_id_type=MESH,
        )

    def send(family, key, src, dst, to, note=True):
        remote(family, key, src, dst, to).start()
        if note:
            held[family] = held.get(family, 0) + bytes_of(src)

    def arrive(key, dst):
        pltpu.make_async_copy(dst, dst, recv_sem.at[names(*key)]).wait()

    def all_sent(family, ref):
        assert held.pop(family) == bytes_of(ref), family
        pltpu.make_async_copy(ref, ref, send_sem.at[families(family)]).wait()

    peers = [dev(other=True)]
    peers += [dev(dy=k) for k in range(1, NY)]
    peers += [dev(dx=k) for k in range(1, NX)]
    peers += [dev(dz=k) for k in range(1, NZ)]
    barrier = pltpu.get_barrier_semaphore()
    for p in peers:
        pl.semaphore_signal(barrier, inc=1, device_id=p, device_id_type=MESH)

    local = Names()

    def load(name, src, dst):
        pltpu.make_async_copy(src, dst, loc_sem.at[local(name)]).start()

    def loaded(name, ref):
        pltpu.make_async_copy(ref, ref, loc_sem.at[local(name)]).wait()

    load("gate", gate_hbm.at[0], gatev)
    load("up", up_hbm.at[0], upv)
    load("cot", cot_hbm.at[0], cotv)
    off = pl.multiple_of(h * ROWS, ROWS)
    load("mixd", mix_hbm.at[:, pl.ds(off, ROWS), pl.ds(off, ROWS)], mixd)
    load("mixo", mix_hbm.at[:, pl.ds(ROWS, ROWS), pl.ds(0, ROWS)], mixo)

    def columns(block):
        return pl.ds(pl.multiple_of(block * ROWS, ROWS), ROWS)

    for k in range(NY):
        load("x", x_hbm.at[0, :, columns(2 * k + c)], xo.at[k])
    load("w", wu_hbm, wb.at[dp, 0])
    load("w", wg_hbm, wb.at[dp, 1])

    def gate_rows(i, _):
        rows = pl.ds(pl.multiple_of(i * RB, RB), RB)
        a = gatev[rows, :].astype(f32)
        cdf = 0.5 * (1.0 + lax.erf(a * root_half))
        act = a * cdf
        centered = act - jnp.mean(act, axis=-1, keepdims=True)
        inv = lax.rsqrt(jnp.mean(centered * centered, axis=-1, keepdims=True) + norm_eps)
        normed = centered * inv
        nrm[rows, :] = normed
        si[rows, :] = inv * (cdf + a * jnp.exp(-0.5 * a * a) * root_twopi)
        value = (normed * gainv[...]).astype(bf16)
        for g in range(NG):
            mixin[0, g, rows, :] = value[:, g * CH : (g + 1) * CH]
        return 0

    def up_rows(i, _):
        rows = pl.ds(pl.multiple_of(i * RB, RB), RB)
        a = upv[rows, :].astype(f32)
        ct = cotv[rows, :].astype(f32)
        cdf = 0.5 * (1.0 + lax.erf(a * root_half))
        value = (ct * (a * cdf)).astype(bf16)
        slope = ct * (cdf + a * jnp.exp(-0.5 * a * a) * root_twopi)
        for g in range(NG):
            mixin[1, g, rows, :] = value[:, g * CH : (g + 1) * CH]
            cs[g, rows, :] = slope[:, g * CH : (g + 1) * CH]
        return 0

    def gate_side():
        loaded("gate", gatev)
        lax.fori_loop(0, ROWS // RB, gate_rows, 0, unroll=4)

    def up_side():
        loaded("up", upv)
        loaded("cot", cotv)
        lax.fori_loop(0, ROWS // RB, up_rows, 0)

    pl.when(h == 0)(gate_side)
    pl.when(h == 1)(up_side)
    pl.semaphore_wait(barrier, len(peers))

    order = [zi(v) for v in (4, 3, -3, 2, -2, 1, -1, 0)]
    for j, g in enumerate(order):
        send("pair", ("pair", j), mixin.at[h, g], peer.at[j], pair_dev)

    mine = {0: wu_hbm, 1: wg_hbm}
    for d, parts in ((1, (0, 1)), (-1, (1, 0))):
        for part in parts:
            send("w", ("w", d, part), mine[part], wb.at[dp, part], dev(dy=d))
    for k in range(NY):
        send("xp", ("xp",), x_hbm.at[0, :, columns(2 * k + 1 - c)], xp.at[k], dev(other=True))

    pl.when(h == 0)(up_side)
    pl.when(h == 1)(gate_side)

    def block_of(dy, other=False):
        return yi(dy) * 2 + (1 - c if other else c)

    def weights_own():
        for part in range(2):
            send("wc", ("wc", 0), mine[part], wb.at[dp, part], dev(other=True))

    def weights_first():
        for d, part in ((1, 0), (-1, 1)):
            b = block_of(-d)
            arrive(("w", d, part), wb.at[b, part])
            send("wc", ("wc", -d), wb.at[b, part], wb.at[b, part], dev(other=True))

    def weights_pass(f):
        rows = pl.ds(f * 64, 64)
        for d, part in ((1, 0), (-1, 1)):
            b = block_of(-d)
            send("wf", ("wf", f), wb.at[b, part, rows], wb.at[b, part, rows], dev(dy=d))

    def weights_second():
        for d, part in ((1, 1), (-1, 0)):
            b = block_of(-d)
            arrive(("w", d, part), wb.at[b, part])
            send("wc", ("wc", -d), wb.at[b, part], wb.at[b, part], dev(other=True))

    def weights_third(f):
        b, rows = block_of(2), pl.ds(f * 64, 64)
        arrive(("wf", f), wb.at[b, :, rows])
        send("wc", ("wc", 2), wb.at[b, :, rows], wb.at[b, :, rows], dev(other=True))

    def weights_other(dy):
        b = block_of(dy, True)
        arrive(("wc", dy), wb.at[b])

    own, theirs = pl.ds(0, ROWS), pl.ds(ROWS, ROWS)
    loaded("mixd", mixd)
    loaded("mixo", mixo)
    seg_t = lax.broadcasted_iota(jnp.int32, (ROWS, ROWS), 0) // SEG
    seg_s = lax.broadcasted_iota(jnp.int32, (ROWS, ROWS), 1) // SEG
    keep = seg_s <= seg_t

    def diag(g):
        return jnp.where(keep, mixd[g].astype(f32), 0.0)

    def up_grad(g, spatial):
        gu[g, 0:ROWS, :] = (spatial.astype(bf16).astype(f32) * cs[g]).astype(bf16)

    def share_up(j):
        g = order[j]
        send("gu", ("gu", j), gu.at[g, own], gu.at[g, theirs], dev(other=True), note=False)

    def up_here(j):
        g = order[j]
        arrive(("gu", j), gu.at[g, theirs])

    def gate_grads():
        def rows_of(i, _):
            rows = pl.ds(pl.multiple_of(i * RB, RB), RB)
            nb = jnp.concatenate([back[g, rows, :] for g in range(NG)], axis=1)
            scaled = nb.astype(f32) * gainv[...]
            normed = nrm[rows, :]
            m1 = jnp.mean(scaled, axis=-1, keepdims=True)
            m2 = jnp.mean(scaled * normed, axis=-1, keepdims=True)
            grad = ((scaled - m1 - normed * m2) * si[rows, :]).astype(bf16)
            for g in range(NG):
                gg[g, rows, :] = grad[:, g * CH : (g + 1) * CH]
            return 0

        lax.fori_loop(0, ROWS // RB, rows_of, 0, unroll=4)
        send("gg", ("gg",), gg.at[:, own, :], gg.at[:, theirs, :], dev(other=True), note=False)

    @pl.when(h == 0)
    def _():
        def step(g, _):
            d = diag(g)
            up_grad(g, dot(d.astype(bf16), mixin[0, g]))
            acc[g] = dot(d.T.astype(bf16), mixin[1, g])
            return 0

        lax.fori_loop(0, NG, step, 0)
        for j in range(NG):
            share_up(j)

    @pl.when(h == 1)
    def _():
        def step(g, _):
            d = diag(g)
            back[g] = dot(d.T.astype(bf16), mixin[1, g]).astype(bf16)
            acc[g] = dot(d.astype(bf16), mixin[0, g])
            return 0

        lax.fori_loop(0, NG, step, 0)

    loaded("x", xo)
    arrive(("xp",), xp)
    for k in range(NY):
        xt[k, :, 0:ROWS] = xo[k].T
        xt[k, :, ROWS : 2 * ROWS] = xp[k].T

    def pair_step(j):
        g = order[j]
        arrive(("pair", j), peer.at[j])

        @pl.when(h == 0)
        def _():
            back[g] = (acc[g] + dot(mixo[g].astype(f32).T.astype(bf16), peer[j])).astype(bf16)

        @pl.when(h == 1)
        def _():
            up_grad(g, acc[g] + dot(mixo[g], peer[j]))
            share_up(j)

    def late_gate():
        @pl.when(h == 0)
        def _():
            gate_grads()

    def early_gate():
        @pl.when(h == 1)
        def _():
            gate_grads()

    def gate_here():
        arrive(("gg",), gg.at[:, theirs, :])

    def u_term(k, j):
        return dot(xt[k], gu[j])

    def g_term(s):
        return lambda k, j: dot(xt[k], gg[2 * j + s])

    def half_of(d, kind):
        long = 0 if d == 1 else 1
        return long if kind == "L" else 1 - long

    di = {1: 0, -1: 1}

    def fill(dst, slot, term, half, j, add=False):
        for r in range(2):
            t = term(2 * half + r, j)
            if add:
                t = t + dst[slot, r].astype(f32)
            dst[slot, r] = t.astype(bf16)

    def u_slot(d, kind, k):
        return di[d] * 7 + (k if kind == "L" else 4 + k)

    def chain_key(name, d, kind, k):
        return (name, d, kind, k) if k else (name, 0)

    def u_start(kind, dist, directions=(1, -1)):
        for d in directions:
            slot = di[d] * 2 + (0 if kind == "L" else 1)
            fill(uorg, slot, u_term, half_of(d, kind), zi(d * dist))
            send("u", chain_key("u", d, kind, dist - 1), uorg.at[slot], urec.at[u_slot(d, kind, dist - 1)], dev(dz=d))

    def u_step(kind, k):
        for d in (1, -1):
            slot = u_slot(d, kind, k)
            arrive(("u", d, kind, k), urec.at[slot])
            fill(urec, slot, u_term, half_of(d, kind), zi(d * k), add=True)
            send("u", chain_key("u", d, kind, k - 1), urec.at[slot], urec.at[u_slot(d, kind, k - 1)], dev(dz=d))

    def g_slot(s, d, kind, k):
        return s * 6 + di[d] * 3 + (k if kind == "L" else 2)

    def g_start(s, kind, dist):
        for d in (1, -1):
            slot = s * 4 + di[d] * 2 + (0 if kind == "L" else 1)
            fill(gorg, slot, g_term(s), half_of(d, kind), xi(d * dist))
            send("g", chain_key(("g", s), d, kind, dist - 1), gorg.at[slot], grec.at[g_slot(s, d, kind, dist - 1)], dev(dx=d))

    def g_step(s):
        for d in (1, -1):
            slot = g_slot(s, d, "L", 1)
            arrive(chain_key(("g", s), d, "L", 1), grec.at[slot])
            fill(grec, slot, g_term(s), half_of(d, "L"), xi(d), add=True)
            send("g", chain_key(("g", s), d, "L", 0), grec.at[slot], grec.at[g_slot(s, d, "L", 0)], dev(dx=d))

    def y_slot(d, kind, k):
        return di[d] * 3 + (k if kind == "L" else 2)

    def y_rows(d, kind):
        return pl.ds(half_of(d, kind) * 128, 128)

    def close(s, rec, slot_of, key, term, j):
        arrive(key, rec.at[pl.ds(0, 4)])
        for half in range(2):
            plus = slot_of(1, "L" if half == 0 else "S")
            minus = slot_of(-1, "L" if half == 1 else "S")
            for r in range(2):
                k = 2 * half + r
                t = term(k, j) + rec[plus, r].astype(f32) + rec[minus, r].astype(f32)
                redf[s, k] = t
                redb[s, k] = t.astype(bf16)
        for kind, dist in (("L", 2), ("S", 1)):
            for d in (1, -1):
                rows = y_rows(d, kind)
                send("y", chain_key(("y", s), d, kind, dist - 1), redb.at[s, yi(d * dist), rows], yrec.at[s, y_slot(d, kind, dist - 1)], dev(dy=d))

    def u_end():
        close(2, urec, lambda d, kind: u_slot(d, kind, 0), ("u", 0), u_term, z)

    def g_end(s):
        close(s, grec, lambda d, kind: g_slot(s, d, kind, 0), (("g", s), 0), g_term(s), x)

    def y_step(s):
        for d in (1, -1):
            slot, rows = y_slot(d, "L", 1), y_rows(d, "L")
            arrive(chain_key(("y", s), d, "L", 1), yrec.at[s, slot])
            yrec[s, slot] = (yrec[s, slot].astype(f32) + redf[s, yi(d), rows, :]).astype(bf16)
            send("y", chain_key(("y", s), d, "L", 0), yrec.at[s, slot], yrec.at[s, y_slot(d, "L", 0)], dev(dy=d))

    def y_sum(s):
        arrive((("y", s), 0), yrec.at[s, pl.ds(0, 4)])
        for half in range(2):
            plus = y_slot(1, "L" if half == 0 else "S", 0)
            minus = y_slot(-1, "L" if half == 1 else "S", 0)
            rows = pl.ds(half * 128, 128)
            t = redf[s, y, rows, :] + yrec[s, plus].astype(f32) + yrec[s, minus].astype(f32)
            subf[s, rows, :] = t
            subb[s, rows, :] = t.astype(bf16)

    def rows64(v):
        return pl.ds(pl.multiple_of(v * 64, 64), 64)

    def rows32(v):
        return pl.ds(pl.multiple_of(v * 32, 32), 32)

    def y_end(s):
        y_sum(s)
        if s == 2:
            for k in range(1, NX):
                send("ux", ("ux",), subb.at[2, rows64(xi(k))], ux.at[k - 1], dev(dx=k))
        else:
            for k in range(1, NZ):
                send("gz", ("gz", s), subb.at[s, rows32(zi(k))], gz.at[s, k - 1], dev(dz=k))

    def piece_u():
        arrive(("ux",), ux)
        t = subf[2, rows64(x), :]
        for k in range(1, NX):
            t = t + ux[k - 1].astype(f32)
        agu[x, z] = t.astype(bf16)
        for k in range(1, NZ):
            send("au", ("a", 2), agu.at[x, z], agu.at[x, z], dev(dz=k))

    def piece_g(s):
        arrive(("gz", s), gz.at[s])
        t = subf[s, rows32(z), :]
        for k in range(1, NZ):
            t = t + gz[s, k - 1].astype(f32)
        agg[s, x, z] = t.astype(bf16)
        for k in range(1, NZ):
            send("ag", ("a", s), agg.at[s, x, z], agg.at[s, x, z], dev(dz=k))

    def gathered(s):
        return agu if s == 2 else agg.at[s]

    def gather_z(s):
        buf = gathered(s)
        arrive(("a", s), buf.at[0, pl.ds(0, NZ - 1)])
        for d in (1, -1):
            send("axu" if s == 2 else "axg", ("ax", s, d), buf.at[x], buf.at[x], dev(dx=d))

    def part_of(d):
        return pl.ds(0, NZ // 2) if d == 1 else pl.ds(NZ // 2, NZ // 2)

    def gather_x(s):
        buf = gathered(s)
        for d in (1, -1):
            arrive(("ax", s, d), buf.at[xi(-d)])
            send("axxu" if s == 2 else "axxg", ("axx", s), buf.at[xi(-d), part_of(d)], buf.at[xi(-d), part_of(d)], dev(dx=d))

    def gather_last(s):
        arrive(("axx", s), gathered(s).at[xi(2)])

    def out_block(b):
        lu = jnp.concatenate([gu[g, 0:ROWS, :] for g in range(NG)], axis=1)
        lg = jnp.concatenate([gg[g, 0:ROWS, :] for g in range(NG)], axis=1)
        ig_out[:, columns(b)] = (dot_t(lu, wb[b, 0]) + dot_t(lg, wb[b, 1])).astype(bf16)

    def put_up():
        for i in range(NX):
            for j in range(NZ):
                du_out[i * 64 : (i + 1) * 64, j * CH : (j + 1) * CH] = agu[i, j]

    def put_gate():
        for s in range(2):
            for i in range(NX):
                for j in range(NZ):
                    at = (2 * i + s) * CH
                    dg_out[j * 32 : (j + 1) * 32, at : at + CH] = agg[s, i, j]

    def finish_waits():
        held["gu"], held["gg"] = bytes_of(gu.at[:, own]), bytes_of(gg.at[:, own])
        for family, ref in (
            ("pair", mixin.at[0]), ("w", wb.at[pl.ds(0, 2)]), ("xp", xp), ("wc", wb.at[pl.ds(0, 4)]), ("wf", wb.at[0]),
            ("gu", gu.at[:, own]), ("gg", gg.at[:, own]), ("u", urec), ("g", grec), ("y", yrec), ("ux", ux), ("gz", gz),
            ("au", agu.at[0, pl.ds(0, NZ - 1)]), ("ag", agg.at[:, 0, pl.ds(0, NZ - 1)]),
            ("axu", agu.at[pl.ds(0, 2)]), ("axg", agg.at[:, pl.ds(0, 2)]), ("axxu", agu.at[0]), ("axxg", agg.at[:, 0]),
        ):
            all_sent(family, ref)
        assert not held

    pair_step(0)
    up_here(0)
    u_start("L", 4)
    pair_step(1)
    pair_step(2)
    up_here(1)
    u_start("S", 3, (1,))
    up_here(2)
    u_start("S", 3, (-1,))
    pair_step(3)
    pair_step(4)
    u_step("L", 3)
    pair_step(5)
    early_gate()
    pair_step(6)
    up_here(3)
    up_here(4)
    u_step("S", 2)
    pair_step(7)
    late_gate()
    gate_here()
    g_start(0, "L", 2)
    g_start(0, "S", 1)
    weights_own()
    up_here(5)
    up_here(6)
    up_here(7)
    u_step("L", 2)
    g_start(1, "L", 2)
    weights_first()
    weights_pass(0)
    u_step("S", 1)
    g_step(0)
    g_start(1, "S", 1)
    u_step("L", 1)
    loaded("w", wb.at[dp])
    out_block(block_of(0))
    weights_other(0)
    out_block(block_of(0, True))
    g_step(1)
    weights_second()
    u_end()
    g_end(0)
    out_block(block_of(1))
    y_step(2)
    y_step(0)
    g_end(1)
    y_end(2)
    y_end(0)
    out_block(block_of(3))
    y_step(1)
    weights_pass(1)
    piece_u()
    piece_g(0)
    y_end(1)
    weights_pass(2)
    weights_pass(3)
    weights_other(1)
    out_block(block_of(1, True))
    gather_z(2)
    gather_z(0)
    piece_g(1)
    weights_other(-1)
    out_block(block_of(3, True))
    gather_x(2)
    gather_x(0)
    weights_third(0)
    gather_z(1)
    weights_third(1)
    gather_last(2)
    put_up()
    weights_third(2)
    weights_third(3)
    out_block(block_of(2))
    gather_x(1)
    gather_last(0)
    weights_other(2)
    out_block(block_of(2, True))
    gather_last(1)
    put_gate()
    finish_waits()
    assert (len(families.at), len(names.at), len(local.at)) == (N_SEND, N_RECV, N_LOCAL), (len(families.at), len(names.at), len(local.at))


def on_device(inputs, up_pre, gate_pre, cotangent, norm_gain, up_weight, gate_weight, mix_weight):
    V = pltpu.VMEM
    scratch = [
        V((ROWS, GATED), bf16), V((ROWS, GATED), bf16), V((ROWS, GATED), bf16),
        V((NY, ROWS, ROWS), bf16), V((NY, ROWS, ROWS), bf16), V((NY, ROWS, 2 * ROWS), bf16),
        V((NG, ROWS, ROWS), bf16), V((NG, ROWS, ROWS), bf16),
        V((2, NG, ROWS, CH), bf16), V((NG, ROWS, CH), bf16), V((NG, ROWS, CH), f32), V((NG, ROWS, CH), bf16),
        V((NG, ROWS, CH), f32), V((ROWS, GATED), f32), V((ROWS, GATED), f32),
        V((NG, 2 * ROWS, CH), bf16), V((NG, 2 * ROWS, CH), bf16),
        V((8, 2, ROWS, GATED), bf16),
        V((4, 2, ROWS, CH), bf16), V((14, 2, ROWS, CH), bf16),
        V((8, 2, ROWS, CH), bf16), V((12, 2, ROWS, CH), bf16),
        V((3, NY, ROWS, CH), f32), V((3, NY, ROWS, CH), bf16), V((3, 6, 128, CH), bf16),
        V((3, ROWS, CH), f32), V((3, ROWS, CH), bf16),
        V((3, 64, CH), bf16), V((2, 7, 32, CH), bf16), V((NX, NZ, 64, CH), bf16), V((2, NX, NZ, 32, CH), bf16),
        pltpu.SemaphoreType.DMA((N_SEND,)), pltpu.SemaphoreType.DMA((N_RECV,)),
        pltpu.SemaphoreType.DMA((N_LOCAL,)),
    ]
    anywhere = pl.BlockSpec(memory_space=pl.ANY)
    inside = pl.BlockSpec(memory_space=pltpu.VMEM)
    input_grad, up_grad, gate_grad = pl.pallas_call(
        kernel,
        out_shape=(
            pltpu.VMEM((ROWS, MODEL), bf16),
            pltpu.VMEM((ROWS, GATED), bf16),
            pltpu.VMEM((ROWS, GATED), bf16),
        ),
        in_specs=[anywhere] * 4 + [inside] + [anywhere] * 3,
        out_specs=(inside,) * 3,
        scratch_shapes=scratch,
        compiler_params=pltpu.CompilerParams(
            collective_id=0, has_side_effects=True, vmem_limit_bytes=67043328 - 2097152 - 65536
        ),
    )(
        inputs, up_pre, gate_pre, cotangent, norm_gain.reshape(1, GATED), up_weight, gate_weight, mix_weight,
    )
    hbm = pl.BlockSpec(memory_space=pl.ANY)
    return pl.pallas_call(
        widen,
        out_shape=(
            jax.ShapeDtypeStruct((1, ROWS, MODEL), bf16),
            jax.ShapeDtypeStruct((ROWS, GATED), f32),
            jax.ShapeDtypeStruct((ROWS, GATED), f32),
        ),
        in_specs=[inside] * 3,
        out_specs=(hbm,) * 3,
        scratch_shapes=[V((ROWS, GATED), f32), V((ROWS, GATED), f32), pltpu.SemaphoreType.DMA((5,))],
        compiler_params=pltpu.CompilerParams(vmem_limit_bytes=8 * 1024 * 1024),
    )(input_grad, up_grad, gate_grad)


def widen(ig, du, dg, ig_out, du_out, dg_out, duw, dgw, sem):
    copies = [pltpu.make_async_copy(ig, ig_out.at[0], sem.at[0])]
    copies[0].start()
    half = ROWS // 2
    for k, (src, mid, dst) in enumerate(((du, duw, du_out), (dg, dgw, dg_out))):
        for r in range(2):
            rows = pl.ds(r * half, half)
            mid[rows, :] = src[rows, :].astype(f32) * grad_scale
            copies.append(pltpu.make_async_copy(mid.at[rows], dst.at[rows], sem.at[1 + 2 * k + r]))
            copies[-1].start()
    for copy in copies:
        copy.wait()


def solution(mesh):
    return jax.shard_map(
        on_device,
        mesh=mesh,
        in_specs=(
            P("dp", "sp", None),
            P("dp", "sp", None),
            P("dp", "sp", None),
            P("dp", "sp", None),
            P(),
            P("dp", None),
            P("dp", None),
            P(),
        ),
        out_specs=(P("dp", "sp", None), P("dp", None), P("dp", None)),
        check_vma=False,
    )
```
